32 devices in a mesh: ep: 8 (over z, x), tp: 4 (over y, core).
Axes of the slice: x: 2, y: 2, z: 4, core: 2. Of those that a mesh axis runs over, the one named last changes fastest.
Arguments:
- layer_in: bfloat16 [128, 2048], P('ep'), may hold values from -6 to 6
- state_in: float32 [128, 32, 4096], P('ep', 'tp'), may hold values from -6 to 6
- mix_gain: float32 [2048], replicated, may hold values from 0.1 to 1.9
- rec_weight: bfloat16 [2048, 2048], P('ep', 'tp'), may hold values from -0.125 to 0.125
- key_weight: bfloat16 [2048, 2048], P('ep', 'tp'), may hold values from -0.125 to 0.125
- val_weight: bfloat16 [2048, 2048], P('ep', 'tp'), may hold values from -0.125 to 0.125
- decay_down: bfloat16 [2048, 64], replicated, may hold values from -0.125 to 0.125
- decay_up: bfloat16 [64, 2048], P(None, 'tp'), may hold values from -0.75 to 0.75
- decay_base: float32 [2048], P('tp'), may hold values from -6 to 6
- rate_down: bfloat16 [2048, 64], replicated, may hold values from -0.125 to 0.125
- rate_up: bfloat16 [64, 2048], P(None, 'tp'), may hold values from -0.75 to 0.75
- rate_base: float32 [2048], P('tp'), may hold values from -6 to 6
- key_scale: float32 [2048], P('tp'), may hold values from 0.25 to 4
- group_gain: float32 [2048], P('tp'), may hold values from 0.1 to 1.9
- out_weight: bfloat16 [2048, 2048], P('tp', 'ep'), may hold values from -0.125 to 0.125
- post_gain: float32 [2048], replicated, may hold values from 0.1 to 1.9
- ffn_gain: float32 [2048], replicated, may hold values from 0.1 to 1.9
- routes: int32 [128, 4], P('ep'), may hold values from 0 to 7, all different within a row; in each aligned block of 16 rows (0 to 15, 16 to 31, ...) at most 16 rows name the same one
- route_gates: float32 [128, 4], P('ep'), may hold values from 0.05 to 1
- expert_gate: bfloat16 [8, 2048, 2048], P('ep', None, 'tp'), may hold values from -0.375 to 0.375
- expert_up: bfloat16 [8, 2048, 2048], P('ep', None, 'tp'), may hold values from -0.375 to 0.375
- expert_down: bfloat16 [8, 2048, 2048], P('ep', 'tp'), may hold values from -0.125 to 0.125
- out_gain: float32 [2048], replicated, may hold values from 0.1 to 1.9
Outputs:
- layer_out: bfloat16 [128, 2048], P('ep')
- new_state: float32 [128, 32, 4096], P('ep', 'tp')
The draws below stay inside these ranges and needn't reach their ends.
Inputs may be any that keep to these rules, and one draw needn't show every extreme that they name: `routes`: each row names 4 different experts. Within the rows of one device (aligned blocks of 16 rows) no expert is named by more than 16 rows, and in every draw some block names some expert exactly 16 times.
All inputs are finite; a program needn't handle non-finite values.
Results may differ from the reference program's by a relative error of at most 0.017.
Values may be sent and summed in bfloat16 or wider, within the bound.
A program may use at most 128 MiB of HBM per device.

```python
import math
import jax
import jax.numpy as jnp
import numpy as np
from jax import lax

D = 2048
HEADS = 32
HEAD_DIM = 64
LOW = 64
FF = 2048
TOPK = 4
SEQ_DEV = 16
SEQS = 128
EXPERTS = 8
CAP = 16
N_EP = 8
N_TP = 4


def shard_levels(stream_key, shape, pieces, smallest, largest):
    def one(position, blocks):
        steps = jax.random.uniform(jax.random.fold_in(jax.random.fold_in(stream_key, 6), position), (blocks,), jnp.float32, smallest / len(pieces), largest / len(pieces))
        return jnp.repeat(jnp.exp(steps), shape[position] // blocks).reshape((-1,) + (1,) * (len(shape) - position - 1))

    factor_of = one(*pieces[0])
    for cut in pieces[1:]:
        factor_of = factor_of * one(*cut)
    return factor_of


def routed_block(own_key, own, number, rows, amount, top, limit, slope):
    ranking = jax.random.permutation(own_key, amount)
    packed, common = shares(amount, rows * top, limit, slope, True), shares(amount, rows * top, limit, slope, False)
    places = jnp.arange(amount)

    def named(sizes, turn):
        used = int((sizes > 0).sum())
        fixed = max(1, used // 4)
        moved = fixed + (places - fixed + turn * (used - fixed)) % max(1, amount - fixed)
        return jnp.zeros((amount,), jnp.int32).at[ranking[jnp.where(places < fixed, places, moved)]].set(jnp.asarray(sizes, jnp.int32))

    sizes = jnp.where(number % 4 == 0, named(packed, number // 4), named(common, number - number // 4 - 1))
    mixed = jax.random.permutation(jax.random.fold_in(own, 3), amount)
    donor, taker = mixed[0:amount // 2 * 2:2], mixed[1:amount // 2 * 2:2]
    margin = jnp.minimum(sizes[donor] - 1, limit - sizes[taker]) // 2
    margin = jnp.where((donor == ranking[0]) | (taker == ranking[0]) | (sizes[taker] == 0), 0, jnp.maximum(margin, 0))
    moved = jax.random.randint(jax.random.fold_in(own, 4), (amount // 2,), 0, 1 << 20) % (margin + 1)
    sizes = sizes.at[donor].add(-moved).at[taker].add(moved)
    items = jnp.searchsorted(jnp.cumsum(sizes), jnp.arange(rows * top), side="right").astype(jnp.int32)
    grid = items.reshape(top, rows).T
    grid = grid[jax.random.permutation(jax.random.fold_in(own, 1), rows)]
    turn = jax.random.randint(jax.random.fold_in(own, 2), (rows, 1), 0, top)
    return jnp.take_along_axis(grid, (jnp.arange(top)[None, :] + turn) % top, axis=1)


def shares(number_of, total, most, slope, full):
    loads = [(1 << 20) // math.isqrt(grade ** slope) + 1 for grade in range(1, number_of + 1)]
    largest = most if full else min(most, max(-(-total // number_of), total * loads[0] // sum(loads)))
    least = 1 if total - largest >= number_of - 1 else 0
    counts, rest = [largest] + [least] * (number_of - 1), total - largest - least * (number_of - 1)
    while rest > 0:
        candidates = [i for i in range(1, number_of) if counts[i] < largest] or [i for i in range(1, number_of) if counts[i] < most]
        mass, budget = sum([loads[i] for i in candidates]), rest
        for i in candidates:
            extra = min(most - counts[i], max(1, budget * loads[i] // mass), rest)
            counts[i] = counts[i] + extra
            rest = rest - extra
    return np.array(counts)


def bell_draw(stream_key, extent, spread, limit, shards=(), kind=jnp.bfloat16):
    entries = jax.random.normal(stream_key, extent, jnp.float32) * spread
    if len(shards) > 0:
        entries = shard_levels(stream_key, extent, shards, -0.22, 0.18) * entries
    return jnp.clip(entries, min=-limit, max=limit).astype(kind)


def setup_inputs(seed: int = 0) -> dict:
    seeds = jax.random.split(jax.random.key(seed), 24)
    layer_in = bell_draw(seeds[0], (SEQS, D), 1.0, 6.0, ((0, 8),))
    state_in = bell_draw(seeds[1], (SEQS, HEADS, HEAD_DIM * HEAD_DIM), 1.0, 6.0, ((0, 8), (1, 4)), jnp.float32)
    mix_gain = jnp.clip(1.0 + 0.18 * jax.random.normal(seeds[2], (D,), jnp.float32), 0.1, 1.9)
    rec_weight = bell_draw(seeds[3], (D, D), D ** -0.5, 0.125, ((0, 8), (1, 4)))
    key_weight = bell_draw(seeds[4], (D, D), D ** -0.5, 0.125, ((0, 8), (1, 4)))
    val_weight = bell_draw(seeds[5], (D, D), D ** -0.5, 0.125, ((0, 8), (1, 4)))
    decay_down = bell_draw(seeds[6], (D, LOW), D ** -0.5, 0.125)
    decay_up = bell_draw(seeds[7], (LOW, D), LOW ** -0.5, 0.75, ((1, 4),))
    decay_base = bell_draw(seeds[8], (D,), 1.5, 6.0, ((0, 4),), jnp.float32)
    rate_down = bell_draw(seeds[9], (D, LOW), D ** -0.5, 0.125)
    rate_up = bell_draw(seeds[10], (LOW, D), LOW ** -0.5, 0.75, ((1, 4),))
    rate_base = bell_draw(seeds[11], (D,), 1.0, 6.0, ((0, 4),), jnp.float32)
    key_scale = jnp.clip(jnp.exp(math.log(4.0) - 2.7725887 * jax.random.uniform(seeds[12], (D,), jnp.float32) ** shard_levels(seeds[12], (D,), ((0, 4),), -0.2, 0.2)), 0.25, 4.0)
    group_gain = jnp.clip(1.0 + 0.18 * jax.random.normal(seeds[13], (D,), jnp.float32), 0.1, 1.9)
    out_weight = bell_draw(seeds[14], (D, D), D ** -0.5, 0.125, ((0, 4), (1, 8)))
    post_gain = jnp.clip(1.0 + 0.18 * jax.random.normal(seeds[15], (D,), jnp.float32), 0.1, 1.9)
    ffn_gain = jnp.clip(1.0 + 0.18 * jax.random.normal(seeds[16], (D,), jnp.float32), 0.1, 1.9)
    routes_keys = jax.random.split(jax.random.fold_in(seeds[17], 1), SEQS // SEQ_DEV)
    routes_turns = jax.random.permutation(jax.random.fold_in(seeds[17], 3), SEQS // SEQ_DEV)
    routes = jax.vmap(lambda own, number: routed_block(jax.random.fold_in(seeds[17], 2), own, number, SEQ_DEV, EXPERTS, TOPK, CAP, 2))(routes_keys, routes_turns).reshape((SEQS, TOPK))
    route_gates = jnp.clip(jnp.exp(math.log(1.0) - 2.9957323 * jax.random.uniform(seeds[18], (SEQS, TOPK), jnp.float32) ** shard_levels(seeds[18], (SEQS, TOPK), ((0, 8),), -0.2, 0.2)), 0.05, 1.0)
    expert_gate = bell_draw(seeds[19], (EXPERTS, D, FF), (D // 9) ** -0.5, 0.375, ((0, 8), (2, 4)))
    expert_up = bell_draw(seeds[20], (EXPERTS, D, FF), (D // 9) ** -0.5, 0.375, ((0, 8), (2, 4)))
    expert_down = bell_draw(seeds[21], (EXPERTS, FF, D), FF ** -0.5, 0.125, ((0, 8), (1, 4)))
    out_gain = jnp.clip(1.0 + 0.18 * jax.random.normal(seeds[22], (D,), jnp.float32), 0.1, 1.9)
    return {"layer_in": layer_in, "state_in": state_in, "mix_gain": mix_gain, "rec_weight": rec_weight, "key_weight": key_weight, "val_weight": val_weight, "decay_down": decay_down, "decay_up": decay_up, "decay_base": decay_base, "rate_down": rate_down, "rate_up": rate_up, "rate_base": rate_base, "key_scale": key_scale, "group_gain": group_gain, "out_weight": out_weight, "post_gain": post_gain, "ffn_gain": ffn_gain, "routes": routes, "route_gates": route_gates, "expert_gate": expert_gate, "expert_up": expert_up, "expert_down": expert_down, "out_gain": out_gain}


norm_eps = 1e-06
group_eps = 0.00064
clamp_limit = 7.0
gate_alpha = 1.702

def rms_scale(values, scales):
    return values * lax.rsqrt(lax.optimization_barrier(jnp.mean(values * values, axis=-1, keepdims=True)) + norm_eps) * scales

def rounded(values):
    return lax.optimization_barrier(values.astype(jnp.bfloat16)).astype(jnp.float32)

def update_block(inputs):
    old_state, unit_key, decay_factor, learn_rate, val_rows, key_rows, rec_rows = inputs
    along_key = lax.optimization_barrier(jnp.sum(old_state * unit_key[:, :, None, :], axis=-1))
    new_state = old_state * decay_factor[:, :, None, :] - along_key[..., None] * (unit_key * learn_rate)[:, :, None, :] + val_rows[..., None] * (key_rows * learn_rate)[:, :, None, :]
    readout = lax.optimization_barrier(jnp.sum(new_state * rec_rows[:, :, None, :], axis=-1))
    return (new_state, readout)

def reference(layer_in, state_in, mix_gain, rec_weight, key_weight, val_weight, decay_down, decay_up, decay_base, rate_down, rate_up, rate_base, key_scale, group_gain, out_weight, post_gain, ffn_gain, routes, route_gates, expert_gate, expert_up, expert_down, out_gain):
    normed_in = rms_scale(layer_in.astype(jnp.float32), mix_gain).astype(jnp.bfloat16)
    rec_full = rounded(jnp.dot(normed_in, rec_weight, preferred_element_type=jnp.float32))
    key_full = rounded(jnp.dot(normed_in, key_weight, preferred_element_type=jnp.float32))
    val_full = rounded(jnp.dot(normed_in, val_weight, preferred_element_type=jnp.float32))
    decay_hidden = jnp.tanh(jnp.dot(normed_in, decay_down, preferred_element_type=jnp.float32)).astype(jnp.bfloat16)
    rate_hidden = jnp.dot(normed_in, rate_down, preferred_element_type=jnp.float32).astype(jnp.bfloat16)
    decay_pre = decay_base + jnp.dot(decay_hidden, decay_up, preferred_element_type=jnp.float32)
    decay_factor = jnp.exp(-jnp.exp(-jax.nn.softplus(-decay_pre) - 0.5))
    learn_rate = jax.nn.sigmoid(rate_base + jnp.dot(rate_hidden, rate_up, preferred_element_type=jnp.float32))
    head_shape = (N_EP, SEQ_DEV, HEADS, HEAD_DIM)
    key_heads = key_full.reshape(head_shape)
    scaled_key = key_heads * key_scale.reshape(HEADS, HEAD_DIM)
    unit_key = scaled_key * lax.rsqrt(lax.optimization_barrier(jnp.sum(scaled_key * scaled_key, axis=-1, keepdims=True)) + norm_eps)
    old_state = state_in.reshape(N_EP, SEQ_DEV, HEADS, HEAD_DIM, HEAD_DIM)
    new_state, readout = lax.map(update_block, (old_state, unit_key, decay_factor.reshape(head_shape), learn_rate.reshape(head_shape), val_full.reshape(head_shape), key_heads, rec_full.reshape(head_shape)))
    readout = readout.reshape(SEQS, HEADS, HEAD_DIM)
    centred = readout - lax.optimization_barrier(jnp.mean(readout, axis=-1, keepdims=True))
    normed_out = centred * lax.rsqrt(lax.optimization_barrier(jnp.mean(centred * centred, axis=-1, keepdims=True)) + group_eps)
    normed_out = (normed_out * group_gain.reshape(HEADS, HEAD_DIM)).reshape(SEQS, D).astype(jnp.bfloat16)
    grouped_out = normed_out.astype(jnp.float32).reshape(SEQS, N_TP, D // N_TP)
    grouped_weight = out_weight.astype(jnp.float32).reshape(N_TP, D // N_TP, D)
    partials = jnp.einsum('sgc,gcd->gsd', grouped_out, grouped_weight)
    mix_sum = lax.optimization_barrier(jnp.sum(rounded(partials), axis=0))
    middle = (layer_in.astype(jnp.float32) + rms_scale(mix_sum, post_gain)).astype(jnp.bfloat16)
    ffn_in = rms_scale(middle.astype(jnp.float32), ffn_gain).astype(jnp.bfloat16)
    flat_routes = routes.reshape(N_EP, SEQ_DEV * TOPK)
    onehot = (flat_routes[:, :, None] == jnp.arange(EXPERTS, dtype=jnp.int32)[None, None, :]).astype(jnp.int32)
    slot_rank = lax.optimization_barrier(jnp.sum((jnp.cumsum(onehot, axis=1) - 1) * onehot, axis=2))
    source = jnp.arange(N_EP, dtype=jnp.int32)[:, None]
    slot_index = (flat_routes * (N_EP * CAP) + source * CAP + slot_rank).reshape(-1).astype(jnp.int32)
    token_index = jnp.arange(SEQS * TOPK, dtype=jnp.int32) // TOPK
    slot_token = jnp.full((EXPERTS * N_EP * CAP,), SEQS, jnp.int32).at[slot_index].set(token_index)
    padded_in = jnp.concatenate([ffn_in, jnp.zeros((1, D), jnp.bfloat16)], axis=0)

    def run_expert(inputs):
        tokens, w_gate, w_up, w_down = inputs
        taken_rows = padded_in[tokens]
        gate_cut = jnp.minimum(jnp.dot(taken_rows, w_gate, preferred_element_type=jnp.float32), clamp_limit)
        up_cut = jnp.clip(jnp.dot(taken_rows, w_up, preferred_element_type=jnp.float32), -clamp_limit, clamp_limit)
        hidden = ((up_cut + 1.0) * gate_cut * jax.nn.sigmoid(gate_alpha * gate_cut)).astype(jnp.bfloat16)
        grouped = hidden.astype(jnp.float32).reshape(tokens.shape[0], N_TP, FF // N_TP)
        down_groups = w_down.astype(jnp.float32).reshape(N_TP, FF // N_TP, D)
        parts = jnp.einsum('rgf,gfd->grd', grouped, down_groups)
        return lax.optimization_barrier(jnp.sum(rounded(parts), axis=0)).astype(jnp.bfloat16)
    expert_rows = lax.map(run_expert, (slot_token.reshape(EXPERTS, N_EP * CAP), expert_gate, expert_up, expert_down))
    picked = expert_rows.reshape(-1, D)[slot_index].reshape(SEQS, TOPK, D)
    moe_sum = lax.optimization_barrier(jnp.sum(route_gates[:, :, None] * picked.astype(jnp.float32), axis=1))
    layer_out = (middle.astype(jnp.float32) + rms_scale(moe_sum, out_gain)).astype(jnp.bfloat16)
    return (layer_out, new_state.reshape(SEQS, HEADS, HEAD_DIM * HEAD_DIM))
```

```python
import functools
import math

import jax
import jax.numpy as jnp
from jax import lax
from jax.experimental import pallas as pl
from jax.experimental.pallas import tpu as pltpu
from jax.sharding import PartitionSpec as P

HEAD_DIM = 64
MESH = pl.DeviceIdType.MESH


norm_eps = 1e-06
group_eps = 0.00064
clamp_limit = 7.0
gate_alpha = 1.702


def rms_scale(values, scales):
    return values * lax.rsqrt(jnp.mean(values * values, axis=-1, keepdims=True) + norm_eps) * scales


def rounded(values):
    return lax.optimization_barrier(values.astype(jnp.bfloat16)).astype(jnp.float32)


def local(
    layer_in,
    state_in,
    mix_gain,
    rec_weight,
    key_weight,
    val_weight,
    decay_down,
    decay_up,
    decay_base,
    rate_down,
    rate_up,
    rate_base,
    key_scale,
    group_gain,
    out_weight,
    post_gain,
    ffn_gain,
    routes,
    route_gates,
    expert_gate,
    expert_up,
    expert_down,
    out_gain,
):
    seq_count = layer_in.shape[0]
    model_width = layer_in.shape[1]
    head_count = state_in.shape[1]
    local_cols = rec_weight.shape[1]
    normed_in = rms_scale(layer_in.astype(jnp.float32), mix_gain).astype(jnp.bfloat16)
    spread_rows = lax.all_to_all(normed_in, "ep", split_axis=1, concat_axis=0, tiled=True)
    joined = jnp.concatenate((rec_weight, key_weight, val_weight), axis=1)
    summed = lax.psum_scatter(
        jnp.dot(spread_rows, joined, preferred_element_type=jnp.float32),
        "ep",
        scatter_dimension=0,
        tiled=True,
    )
    rec_sum = summed[:, :local_cols]
    key_sum = summed[:, local_cols : 2 * local_cols]
    val_sum = summed[:, 2 * local_cols :]
    head_shape = (seq_count, head_count, HEAD_DIM)
    rec_rows = rounded(rec_sum).reshape(head_shape)
    key_rows = rounded(key_sum).reshape(head_shape)
    val_rows = rounded(val_sum).reshape(head_shape)
    decay_hidden = jnp.tanh(
        jnp.dot(normed_in, decay_down, preferred_element_type=jnp.float32)
    ).astype(jnp.bfloat16)
    rate_hidden = jnp.dot(normed_in, rate_down, preferred_element_type=jnp.float32).astype(
        jnp.bfloat16
    )
    decay_pre = decay_base + jnp.dot(decay_hidden, decay_up, preferred_element_type=jnp.float32)
    decay_factor = jnp.exp(-jnp.exp(-jax.nn.softplus(-decay_pre) - 0.5)).reshape(head_shape)
    learn_rate = jax.nn.sigmoid(
        rate_base + jnp.dot(rate_hidden, rate_up, preferred_element_type=jnp.float32)
    ).reshape(head_shape)
    scaled_key = key_rows * key_scale.reshape(head_count, HEAD_DIM)
    unit_key = scaled_key * lax.rsqrt(
        jnp.sum(scaled_key * scaled_key, axis=-1, keepdims=True) + norm_eps
    )
    old_state = state_in.reshape(seq_count, head_count, HEAD_DIM, HEAD_DIM)
    along_key = jnp.sum(old_state * unit_key[:, :, None, :], axis=-1)
    new_state = (
        old_state * decay_factor[:, :, None, :]
        - along_key[..., None] * (unit_key * learn_rate)[:, :, None, :]
        + val_rows[..., None] * (key_rows * learn_rate)[:, :, None, :]
    )
    readout = jnp.sum(new_state * rec_rows[:, :, None, :], axis=-1)
    centred = readout - jnp.mean(readout, axis=-1, keepdims=True)
    normed_out = centred * lax.rsqrt(
        jnp.mean(centred * centred, axis=-1, keepdims=True) + group_eps
    )
    normed_out = (
        (normed_out * group_gain.reshape(head_count, HEAD_DIM))
        .reshape(seq_count, local_cols)
        .astype(jnp.bfloat16)
    )
    head_partial = jnp.dot(
        normed_out,
        lax.all_gather(out_weight, "ep", axis=1, tiled=True),
        preferred_element_type=jnp.float32,
    )
    mix_sum = lax.psum(head_partial.astype(jnp.bfloat16), "tp").astype(jnp.float32)
    middle = (layer_in.astype(jnp.float32) + rms_scale(mix_sum, post_gain)).astype(jnp.bfloat16)
    ffn_in = rms_scale(middle.astype(jnp.float32), ffn_gain).astype(jnp.bfloat16)
    top_count = routes.shape[1]
    local_experts = expert_gate.shape[0]
    expert_total = lax.axis_size("ep") * local_experts
    capacity = max(2, 2 * seq_count * top_count // expert_total)
    slot_total = expert_total * capacity
    flat_routes = routes.reshape(-1)
    onehot = (flat_routes[:, None] == jnp.arange(expert_total, dtype=jnp.int32)[None, :]).astype(
        jnp.int32
    )
    slot_rank = jnp.sum((jnp.cumsum(onehot, axis=0) - 1) * onehot, axis=1)
    slot_index = flat_routes * capacity + slot_rank
    slot_range = jnp.arange(slot_total, dtype=jnp.int32)
    dispatch_table = jnp.sum(
        (slot_range[:, None] == slot_index[None, :])
        .astype(jnp.bfloat16)
        .reshape(slot_total, seq_count, top_count),
        axis=2,
    )
    send_rows = jnp.dot(dispatch_table, ffn_in, preferred_element_type=jnp.float32).astype(
        jnp.bfloat16
    )
    send_rows = send_rows.reshape(lax.axis_size("ep"), local_experts, capacity, model_width)
    arrived = lax.all_to_all(send_rows, "ep", split_axis=0, concat_axis=0, tiled=True)
    gate_cut = jnp.minimum(
        jnp.einsum("seid,edf->seif", arrived, expert_gate, preferred_element_type=jnp.float32),
        clamp_limit,
    )
    up_cut = jnp.clip(
        jnp.einsum("seid,edf->seif", arrived, expert_up, preferred_element_type=jnp.float32),
        -clamp_limit,
        clamp_limit,
    )
    hidden = ((up_cut + 1.0) * gate_cut * jax.nn.sigmoid(gate_alpha * gate_cut)).astype(
        jnp.bfloat16
    )
    partial_value = jnp.einsum(
        "seif,efd->seid", hidden, expert_down, preferred_element_type=jnp.float32
    )
    returned = lax.psum(partial_value.astype(jnp.bfloat16), "tp")
    back_rows = lax.all_to_all(returned, "ep", split_axis=0, concat_axis=0, tiled=True)
    back_flat = back_rows.reshape(slot_total, model_width)
    combine_table = (slot_index[:, None] == slot_range[None, :]).astype(jnp.bfloat16)
    picked = jnp.dot(combine_table, back_flat, preferred_element_type=jnp.float32)
    moe_sum = jnp.sum(
        route_gates[:, :, None] * picked.reshape(seq_count, top_count, model_width), axis=1
    )
    layer_out = (middle.astype(jnp.float32) + rms_scale(moe_sum, out_gain)).astype(jnp.bfloat16)
    return (layer_out, new_state.reshape(seq_count, head_count, HEAD_DIM * HEAD_DIM))


def power_of_two(value):
    return value > 0 and value & (value - 1) == 0


def row_scale(values):
    return values * lax.rsqrt(jnp.mean(values * values, axis=-1, keepdims=True) + norm_eps)


def layer_kernel(
    n,
    m,
    layer_in,
    mix_gain,
    decay_base,
    rate_base,
    key_scale,
    group_gain,
    post_gain,
    ffn_gain,
    out_gain,
    routes,
    route_gates,
    state_hbm,
    rec_hbm,
    key_hbm,
    val_hbm,
    ddown_hbm,
    dup_hbm,
    rdown_hbm,
    rup_hbm,
    out_hbm,
    egate_hbm,
    eup_hbm,
    edown_hbm,
    layer_out,
    new_state,
    state_v,
    proj_v,
    ddown_v,
    dup_v,
    rdown_v,
    rup_v,
    out_v,
    egate_v,
    eup_v,
    edown_v,
    spread_v,
    gather_t,
    products,
    fresh_v,
    s1,
    r1,
    s2,
    r2,
    a3,
    s4,
    p5,
    f6,
    a6,
    s7,
    r7,
    s8,
    r8,
    a9,
    local_sem,
    ep_send,
    ep_recv,
    tp_send,
    tp_recv,
    fw_send,
    fw_recv,
):
    e = lax.axis_index("ep")
    t = lax.axis_index("tp")
    seqs, width = layer_in.shape
    heads = state_hbm.shape[1]
    flat = state_hbm.shape[2]
    cols = rec_hbm.shape[1]
    rows = rec_hbm.shape[0]
    pairs = seqs * heads
    tokens = n * seqs
    f32 = jnp.float32
    bf16 = jnp.bfloat16

    loads = [
        pltpu.make_async_copy(source, target, local_sem.at[i])
        for i, (source, target) in enumerate(
            (
                (ddown_hbm, ddown_v),
                (rdown_hbm, rdown_v),
                (dup_hbm, dup_v),
                (rup_hbm, rup_v),
                (rec_hbm, proj_v.at[0]),
                (key_hbm, proj_v.at[1]),
                (val_hbm, proj_v.at[2]),
                (state_hbm, state_v),
                (out_hbm, out_v),
                (egate_hbm.at[0], egate_v),
                (eup_hbm.at[0], eup_v),
                (edown_hbm.at[0], edown_v),
            )
        )
    ]
    barrier = pltpu.get_barrier_semaphore()
    for d in range(1, n):
        pl.semaphore_signal(barrier, inc=1, device_id=(lax.rem(e + d, n), t), device_id_type=MESH)
    for d in range(1, m):
        pl.semaphore_signal(barrier, inc=1, device_id=(e, lax.rem(t + d, m)), device_id_type=MESH)
    for load in loads:
        load.start()

    def ep_copy(phase, d, source, target):
        return pltpu.make_async_remote_copy(
            src_ref=source,
            dst_ref=target,
            send_sem=ep_send.at[phase, d],
            recv_sem=ep_recv.at[phase, d],
            device_id=(lax.rem(e + d, n), t),
            device_id_type=MESH,
        )

    def tp_copy(phase, d, source, target):
        return pltpu.make_async_remote_copy(
            src_ref=source,
            dst_ref=target,
            send_sem=tp_send.at[phase, d],
            recv_sem=tp_recv.at[phase, d],
            device_id=(e, lax.rem(t + d, m)),
            device_id_type=MESH,
        )

    sent = []

    def start(copies):
        for copy in copies:
            copy.start()
        sent.extend(copies)
        return copies

    token_in = layer_in[...].astype(f32)
    normed = (row_scale(token_in) * mix_gain[...]).astype(bf16)
    for j in range(n):
        s1[j] = normed[:, j * rows : (j + 1) * rows]
    r1[e] = s1[e]
    pl.semaphore_wait(barrier, n - 1 + m - 1)
    first = start([ep_copy(0, d, s1.at[lax.rem(e + d, n)], r1.at[e]) for d in range(1, n)])

    for load in loads[:4]:
        load.wait()
    decay_hidden = jnp.tanh(jnp.dot(normed, ddown_v[...], preferred_element_type=f32)).astype(bf16)
    rate_hidden = jnp.dot(normed, rdown_v[...], preferred_element_type=f32).astype(bf16)
    decay_pre = decay_base[...] + jnp.dot(decay_hidden, dup_v[...], preferred_element_type=f32)
    rate_pre = rate_base[...] + jnp.dot(rate_hidden, rup_v[...], preferred_element_type=f32)
    scale_wide = jnp.broadcast_to(key_scale[...], (seqs, cols))

    def head_major(values):
        return jnp.concatenate(
            [values[:, h * HEAD_DIM : (h + 1) * HEAD_DIM] for h in range(heads)], axis=0
        )

    head_bits = int(math.log2(heads))
    seq_bits = int(math.log2(seqs))
    dim_bits = int(math.log2(HEAD_DIM))
    i0 = lax.broadcasted_iota(jnp.int32, (pairs, pairs), 0)
    i1 = lax.broadcasted_iota(jnp.int32, (pairs, pairs), 1)
    to_pairs = (i1 == ((i0 & (heads - 1)) << seq_bits) + (i0 >> head_bits)).astype(f32)
    from_pairs = (i0 == ((i1 & (heads - 1)) << seq_bits) + (i1 >> head_bits)).astype(bf16)

    side = jnp.concatenate(
        [head_major(decay_pre), head_major(rate_pre), head_major(scale_wide)], axis=1
    )
    side = jnp.dot(to_pairs, side, preferred_element_type=f32, precision=lax.Precision.HIGHEST)
    decay = jnp.exp(jax.nn.sigmoid(side[:, :HEAD_DIM]) * -math.exp(-0.5))
    rate = jax.nn.sigmoid(side[:, HEAD_DIM : 2 * HEAD_DIM])
    scale = side[:, 2 * HEAD_DIM :]
    c0 = lax.broadcasted_iota(jnp.int32, (2 * HEAD_DIM, flat), 0) & (HEAD_DIM - 1)
    c1 = lax.broadcasted_iota(jnp.int32, (2 * HEAD_DIM, flat), 1) >> dim_bits
    spread_v[...] = (c0 == c1).astype(f32).astype(bf16)
    g0 = lax.broadcasted_iota(jnp.int32, (flat, HEAD_DIM), 0) >> dim_bits
    g1 = lax.broadcasted_iota(jnp.int32, (flat, HEAD_DIM), 1)
    gather_t[...] = (g0 == g1).astype(f32).astype(bf16)

    for load in loads[4:7]:
        load.wait()
    for copy in first:
        copy.wait_recv()
    spread_rows = r1[...].reshape(tokens, rows)
    for w in range(3):
        part = jnp.dot(spread_rows, proj_v[w], preferred_element_type=f32).astype(bf16)
        s2[:, :, w * cols : (w + 1) * cols] = part.reshape(n, seqs, cols)
    r2[e] = s2[e]
    second = start([ep_copy(1, d, s2.at[lax.rem(e + d, n)], r2.at[e]) for d in range(1, n)])
    loads[7].wait()
    for copy in second:
        copy.wait_recv()
    total = r2[0].astype(f32)
    for j in range(1, n):
        total = total + r2[j].astype(f32)
    total = total.astype(bf16).astype(f32)
    heads_in = jnp.concatenate(
        [head_major(total[:, w * cols : (w + 1) * cols]) for w in range(3)], axis=1
    ).astype(bf16)
    heads_in = jnp.dot(to_pairs.astype(bf16), heads_in, preferred_element_type=f32)
    rec = heads_in[:, :HEAD_DIM]
    key = heads_in[:, HEAD_DIM : 2 * HEAD_DIM]
    val = heads_in[:, 2 * HEAD_DIM :]
    scaled = key * scale
    unit = scaled * lax.rsqrt(jnp.sum(scaled * scaled, axis=-1, keepdims=True) + norm_eps)
    unit_rate = unit * rate
    key_rate = key * rate
    decay_rec = decay * rec
    along_gain = jnp.sum(unit_rate * rec, axis=-1, keepdims=True)
    val_gain = jnp.sum(key_rate * rec, axis=-1, keepdims=True)

    lanes = 2 * HEAD_DIM
    two = lambda values: jnp.concatenate([values, values], axis=1)
    unit2, decay_rec2 = two(unit), two(decay_rec)

    def products_step(j, carry):
        at = pl.ds(pl.multiple_of(j * lanes, lanes), lanes)
        block = state_v[:, :, at].reshape(pairs, lanes)
        for i, factor in enumerate((unit2, decay_rec2)):
            value = block * factor
            high = value.astype(bf16)
            products[2 * i * pairs : (2 * i + 1) * pairs, at] = high
            products[(2 * i + 1) * pairs : (2 * i + 2) * pairs, at] = (
                value - high.astype(f32)
            ).astype(bf16)
        return carry

    lax.fori_loop(0, flat // lanes, products_step, 0)
    reduced = jnp.dot(products[...], gather_t[...], preferred_element_type=f32)
    along = reduced[:pairs] + reduced[pairs : 2 * pairs]
    readout = (
        reduced[2 * pairs : 3 * pairs] + reduced[3 * pairs :] - along * along_gain + val * val_gain
    )
    centred = readout - jnp.mean(readout, axis=-1, keepdims=True)
    normed_out = centred * lax.rsqrt(jnp.mean(centred * centred, axis=-1, keepdims=True) + group_eps)
    out_high = normed_out.astype(bf16)
    out_low = (normed_out - out_high.astype(f32)).astype(bf16)
    back = jnp.dot(
        from_pairs, jnp.concatenate([out_high, out_low], axis=1), preferred_element_type=f32
    )
    back = back[:, :HEAD_DIM] + back[:, HEAD_DIM:]
    back = jnp.concatenate([back[h * seqs : (h + 1) * seqs] for h in range(heads)], axis=1)
    a3[e] = (back * group_gain[...]).astype(bf16)
    third = start([ep_copy(2, d, a3.at[e], a3.at[e]) for d in range(1, n)])

    along_high = along.astype(bf16)
    along_low = (along - along_high.astype(f32)).astype(bf16)
    along_pair = jnp.concatenate([along_high, along_low], axis=1)
    val_low = val.astype(bf16)
    decay2, unit_rate2, key_rate2 = two(decay), two(unit_rate), two(key_rate)

    def fresh_step(j, carry):
        at = pl.ds(pl.multiple_of(j * lanes, lanes), lanes)
        block = state_v[:, :, at].reshape(pairs, lanes)
        table = spread_v[:, at]
        along_wide = jnp.dot(along_pair, table, preferred_element_type=f32)
        val_wide = jnp.dot(val_low, table[:HEAD_DIM], preferred_element_type=f32)
        fresh = block * decay2 - along_wide * unit_rate2 + val_wide * key_rate2
        fresh_v[:, :, at] = fresh.reshape(seqs, heads, lanes)
        return carry

    lax.fori_loop(0, flat // lanes, fresh_step, 0)
    store = pltpu.make_async_copy(fresh_v, new_state, local_sem.at[len(loads)])
    store.start()

    loads[8].wait()
    for copy in third:
        copy.wait_recv()
    part = jnp.dot(a3[...].reshape(tokens, cols), out_v[...], preferred_element_type=f32)
    s4[...] = part.astype(bf16).reshape(n, seqs, rows)
    p5[t, e] = s4[e]
    fourth = start([ep_copy(3, d, s4.at[lax.rem(e + d, n)], p5.at[t, e]) for d in range(1, n)])
    for copy in fourth:
        copy.wait_recv()
    fifth = start([tp_copy(0, d, p5.at[t], p5.at[t]) for d in range(1, m)])
    for copy in fifth:
        copy.wait_recv()
    mixed = p5[0].astype(f32)
    for q in range(1, m):
        mixed = mixed + p5[q].astype(f32)
    mixed = jnp.concatenate([mixed[j] for j in range(n)], axis=1)
    middle = (token_in + row_scale(mixed) * post_gain[...]).astype(bf16).astype(f32)
    ffn_in = (row_scale(middle) * ffn_gain[...]).astype(bf16)

    for q in range(m):
        f6[q] = ffn_in[:, q * cols : (q + 1) * cols]
        a6[q, e] = ffn_in[:, q * cols : (q + 1) * cols]
    sixth = start([ep_copy(4, d, f6.at[t], a6.at[t, e]) for d in range(1, n)])
    passed = {}
    for d in range(1, n):
        sixth[d - 1].wait_recv()
        source = lax.rem(e + n - d, n)
        for k in range(1, m):
            passed[d, k] = pltpu.make_async_remote_copy(
                src_ref=a6.at[t, source],
                dst_ref=a6.at[t, source],
                send_sem=fw_send.at[d, k],
                recv_sem=fw_recv.at[d, k],
                device_id=(e, lax.rem(t + k, m)),
                device_id_type=MESH,
            )
            start([passed[d, k]])
    for load in loads[9:]:
        load.wait()
    gate = jnp.zeros((tokens, egate_hbm.shape[2]), f32)
    up = gate
    for k in range(m):
        q = lax.rem(t + m - k, m)
        if k > 0:
            for d in range(1, n):
                passed[d, k].wait_recv()
        taken = a6[q].reshape(tokens, cols)
        at = pl.ds(pl.multiple_of(q * cols, cols), cols)
        gate = gate + jnp.dot(taken, egate_v[at, :], preferred_element_type=f32)
        up = up + jnp.dot(taken, eup_v[at, :], preferred_element_type=f32)
    gate = jnp.minimum(gate, clamp_limit)
    up = jnp.clip(up, -clamp_limit, clamp_limit)
    hidden = ((up + 1.0) * gate * jax.nn.sigmoid(gate_alpha * gate)).astype(bf16)

    seventh = []
    for k in [2, 3, 1, 0] if m == 4 else list(range(1, m)) + [0]:
        q = lax.rem(t + k, m)
        at = pl.ds(pl.multiple_of(q * cols, cols), cols)
        part = jnp.dot(hidden, edown_v[:, at], preferred_element_type=f32).astype(bf16)
        if k == 0:
            own = part.astype(f32)
        else:
            s7[q] = part
            seventh += start([tp_copy(1, k, s7.at[q], r7.at[t])])
    for copy in seventh:
        copy.wait_recv()
    for k in range(1, m):
        own = own + r7[lax.rem(t + k, m)].astype(f32)
    s8[...] = own.astype(bf16).reshape(n, seqs, cols)
    r8[e] = s8[e]
    eighth = start([ep_copy(5, d, s8.at[lax.rem(e + d, n)], r8.at[e]) for d in range(1, n)])
    named = routes[...]
    gates = route_gates[...]
    for copy in eighth:
        copy.wait_recv()
    moe = jnp.zeros((seqs, cols), f32)
    for j in range(n):
        weight = jnp.sum(jnp.where(named == j, gates, 0.0), axis=1, keepdims=True)
        moe = moe + weight * r8[j].astype(f32)
    a9[t] = moe
    ninth = start([tp_copy(2, d, a9.at[t], a9.at[t]) for d in range(1, m)])
    for copy in ninth:
        copy.wait_recv()
    moe = jnp.concatenate([a9[q] for q in range(m)], axis=1)
    layer_out[...] = (middle + row_scale(moe) * out_gain[...]).astype(bf16)
    for copy in sent:
        copy.wait_send()
    store.wait()


def fused_local(n, m, *args):
    (
        layer_in, state_in, mix_gain, rec_weight, key_weight, val_weight, decay_down, decay_up,
        decay_base, rate_down, rate_up, rate_base, key_scale, group_gain, out_weight, post_gain,
        ffn_gain, routes, route_gates, expert_gate, expert_up, expert_down, out_gain,
    ) = args
    seqs, width = layer_in.shape
    heads, flat = state_in.shape[1:]
    rows, cols = rec_weight.shape
    low = decay_down.shape[1]
    hidden = expert_gate.shape[2]
    pairs = seqs * heads
    tokens = n * seqs
    f32, bf16 = jnp.float32, jnp.bfloat16
    line = lambda values: values.reshape(1, -1)
    vmem = pl.BlockSpec(memory_space=pltpu.VMEM)
    hbm = pl.BlockSpec(memory_space=pl.ANY)
    dma = pltpu.SemaphoreType.DMA
    return pl.pallas_call(
        functools.partial(layer_kernel, n, m),
        out_shape=(
            jax.ShapeDtypeStruct(layer_in.shape, bf16),
            jax.ShapeDtypeStruct(state_in.shape, f32),
        ),
        in_specs=[vmem] * 11 + [hbm] * 12,
        out_specs=(vmem, hbm),
        scratch_shapes=[
            pltpu.VMEM(state_in.shape, f32),
            pltpu.VMEM((3, rows, cols), bf16),
            pltpu.VMEM((width, low), bf16),
            pltpu.VMEM((low, cols), bf16),
            pltpu.VMEM((width, low), bf16),
            pltpu.VMEM((low, cols), bf16),
            pltpu.VMEM(out_weight.shape, bf16),
            pltpu.VMEM((width, hidden), bf16),
            pltpu.VMEM((width, hidden), bf16),
            pltpu.VMEM((hidden, width), bf16),
            pltpu.VMEM((2 * HEAD_DIM, flat), bf16),
            pltpu.VMEM((flat, HEAD_DIM), bf16),
            pltpu.VMEM((4 * pairs, flat), bf16),
            pltpu.VMEM(state_in.shape, f32),
            pltpu.VMEM((n, seqs, rows), bf16),
            pltpu.VMEM((n, seqs, rows), bf16),
            pltpu.VMEM((n, seqs, 3 * cols), bf16),
            pltpu.VMEM((n, seqs, 3 * cols), bf16),
            pltpu.VMEM((n, seqs, cols), bf16),
            pltpu.VMEM((n, seqs, rows), bf16),
            pltpu.VMEM((m, n, seqs, rows), bf16),
            pltpu.VMEM((m, seqs, cols), bf16),
            pltpu.VMEM((m, n, seqs, cols), bf16),
            pltpu.VMEM((m, tokens, cols), bf16),
            pltpu.VMEM((m, tokens, cols), bf16),
            pltpu.VMEM((n, seqs, cols), bf16),
            pltpu.VMEM((n, seqs, cols), bf16),
            pltpu.VMEM((m, seqs, cols), f32),
            dma((13,)),
            dma((6, n)),
            dma((6, n)),
            dma((3, m)),
            dma((3, m)),
            dma((n, m)),
            dma((n, m)),
        ],
        compiler_params=pltpu.CompilerParams(
            collective_id=0, has_side_effects=True, vmem_limit_bytes=60 * 1024 * 1024
        ),
    )(
        layer_in, line(mix_gain), line(decay_base), line(rate_base), line(key_scale),
        line(group_gain), line(post_gain), line(ffn_gain), line(out_gain), routes, route_gates,
        state_in, rec_weight, key_weight, val_weight, decay_down, decay_up, rate_down, rate_up,
        out_weight, expert_gate, expert_up, expert_down,
    )


def choose(n, m, *args):
    seqs, width = args[0].shape
    heads = args[1].shape[1]
    cols = args[3].shape[1]
    experts = args[19].shape[0]
    capacity = max(2, 2 * seqs * args[17].shape[1] // (n * experts))
    if (
        capacity >= seqs
        and experts == 1
        and power_of_two(seqs)
        and power_of_two(heads)
        and seqs % 16 == 0
        and heads % 8 == 0
        and cols * m == width
    ):
        return fused_local(n, m, *args)
    return local(*args)


def solution(mesh):
    in_specs = (
        P("ep", None),
        P("ep", "tp", None),
        P(),
        P("ep", "tp"),
        P("ep", "tp"),
        P("ep", "tp"),
        P(),
        P(None, "tp"),
        P("tp"),
        P(),
        P(None, "tp"),
        P("tp"),
        P("tp"),
        P("tp"),
        P("tp", "ep"),
        P(),
        P(),
        P("ep", None),
        P("ep", None),
        P("ep", None, "tp"),
        P("ep", None, "tp"),
        P("ep", "tp", None),
        P(),
    )
    out_specs = (P("ep", None), P("ep", "tp", None))
    return jax.shard_map(
        functools.partial(choose, mesh.shape["ep"], mesh.shape["tp"]), mesh=mesh, in_specs=in_specs, out_specs=out_specs, check_vma=False)
```

```python
import functools
import math

import jax
import jax.numpy as jnp
from jax import lax
from jax.experimental import pallas as pl
from jax.experimental.pallas import tpu as pltpu
from jax.sharding import PartitionSpec as P

HEAD_DIM = 64
MESH = pl.DeviceIdType.MESH


norm_eps = 1e-06
group_eps = 0.00064
clamp_limit = 7.0
gate_alpha = 1.702


def rms_scale(values, scales):
    return values * lax.rsqrt(jnp.mean(values * values, axis=-1, keepdims=True) + norm_eps) * scales


def rounded(values):
    return lax.optimization_barrier(values.astype(jnp.bfloat16)).astype(jnp.float32)


def local(
    layer_in,
    state_in,
    mix_gain,
    rec_weight,
    key_weight,
    val_weight,
    decay_down,
    decay_up,
    decay_base,
    rate_down,
    rate_up,
    rate_base,
    key_scale,
    group_gain,
    out_weight,
    post_gain,
    ffn_gain,
    routes,
    route_gates,
    expert_gate,
    expert_up,
    expert_down,
    out_gain,
):
    seq_count = layer_in.shape[0]
    model_width = layer_in.shape[1]
    head_count = state_in.shape[1]
    local_cols = rec_weight.shape[1]
    normed_in = rms_scale(layer_in.astype(jnp.float32), mix_gain).astype(jnp.bfloat16)
    spread_rows = lax.all_to_all(normed_in, "ep", split_axis=1, concat_axis=0, tiled=True)
    joined = jnp.concatenate((rec_weight, key_weight, val_weight), axis=1)
    summed = lax.psum_scatter(
        jnp.dot(spread_rows, joined, preferred_element_type=jnp.float32),
        "ep",
        scatter_dimension=0,
        tiled=True,
    )
    rec_sum = summed[:, :local_cols]
    key_sum = summed[:, local_cols : 2 * local_cols]
    val_sum = summed[:, 2 * local_cols :]
    head_shape = (seq_count, head_count, HEAD_DIM)
    rec_rows = rounded(rec_sum).reshape(head_shape)
    key_rows = rounded(key_sum).reshape(head_shape)
    val_rows = rounded(val_sum).reshape(head_shape)
    decay_hidden = jnp.tanh(
        jnp.dot(normed_in, decay_down, preferred_element_type=jnp.float32)
    ).astype(jnp.bfloat16)
    rate_hidden = jnp.dot(normed_in, rate_down, preferred_element_type=jnp.float32).astype(
        jnp.bfloat16
    )
    decay_pre = decay_base + jnp.dot(decay_hidden, decay_up, preferred_element_type=jnp.float32)
    decay_factor = jnp.exp(-jnp.exp(-jax.nn.softplus(-decay_pre) - 0.5)).reshape(head_shape)
    learn_rate = jax.nn.sigmoid(
        rate_base + jnp.dot(rate_hidden, rate_up, preferred_element_type=jnp.float32)
    ).reshape(head_shape)
    scaled_key = key_rows * key_scale.reshape(head_count, HEAD_DIM)
    unit_key = scaled_key * lax.rsqrt(
        jnp.sum(scaled_key * scaled_key, axis=-1, keepdims=True) + norm_eps
    )
    old_state = state_in.reshape(seq_count, head_count, HEAD_DIM, HEAD_DIM)
    along_key = jnp.sum(old_state * unit_key[:, :, None, :], axis=-1)
    new_state = (
        old_state * decay_factor[:, :, None, :]
        - along_key[..., None] * (unit_key * learn_rate)[:, :, None, :]
        + val_rows[..., None] * (key_rows * learn_rate)[:, :, None, :]
    )
    readout = jnp.sum(new_state * rec_rows[:, :, None, :], axis=-1)
    centred = readout - jnp.mean(readout, axis=-1, keepdims=True)
    normed_out = centred * lax.rsqrt(
        jnp.mean(centred * centred, axis=-1, keepdims=True) + group_eps
    )
    normed_out = (
        (normed_out * group_gain.reshape(head_count, HEAD_DIM))
        .reshape(seq_count, local_cols)
        .astype(jnp.bfloat16)
    )
    head_partial = jnp.dot(
        normed_out,
        lax.all_gather(out_weight, "ep", axis=1, tiled=True),
        preferred_element_type=jnp.float32,
    )
    mix_sum = lax.psum(head_partial.astype(jnp.bfloat16), "tp").astype(jnp.float32)
    middle = (layer_in.astype(jnp.float32) + rms_scale(mix_sum, post_gain)).astype(jnp.bfloat16)
    ffn_in = rms_scale(middle.astype(jnp.float32), ffn_gain).astype(jnp.bfloat16)
    top_count = routes.shape[1]
    local_experts = expert_gate.shape[0]
    expert_total = lax.axis_size("ep") * local_experts
    capacity = max(2, 2 * seq_count * top_count // expert_total)
    slot_total = expert_total * capacity
    flat_routes = routes.reshape(-1)
    onehot = (flat_routes[:, None] == jnp.arange(expert_total, dtype=jnp.int32)[None, :]).astype(
        jnp.int32
    )
    slot_rank = jnp.sum((jnp.cumsum(onehot, axis=0) - 1) * onehot, axis=1)
    slot_index = flat_routes * capacity + slot_rank
    slot_range = jnp.arange(slot_total, dtype=jnp.int32)
    dispatch_table = jnp.sum(
        (slot_range[:, None] == slot_index[None, :])
        .astype(jnp.bfloat16)
        .reshape(slot_total, seq_count, top_count),
        axis=2,
    )
    send_rows = jnp.dot(dispatch_table, ffn_in, preferred_element_type=jnp.float32).astype(
        jnp.bfloat16
    )
    send_rows = send_rows.reshape(lax.axis_size("ep"), local_experts, capacity, model_width)
    arrived = lax.all_to_all(send_rows, "ep", split_axis=0, concat_axis=0, tiled=True)
    gate_cut = jnp.minimum(
        jnp.einsum("seid,edf->seif", arrived, expert_gate, preferred_element_type=jnp.float32),
        clamp_limit,
    )
    up_cut = jnp.clip(
        jnp.einsum("seid,edf->seif", arrived, expert_up, preferred_element_type=jnp.float32),
        -clamp_limit,
        clamp_limit,
    )
    hidden = ((up_cut + 1.0) * gate_cut * jax.nn.sigmoid(gate_alpha * gate_cut)).astype(
        jnp.bfloat16
    )
    partial_value = jnp.einsum(
        "seif,efd->seid", hidden, expert_down, preferred_element_type=jnp.float32
    )
    returned = lax.psum(partial_value.astype(jnp.bfloat16), "tp")
    back_rows = lax.all_to_all(returned, "ep", split_axis=0, concat_axis=0, tiled=True)
    back_flat = back_rows.reshape(slot_total, model_width)
    combine_table = (slot_index[:, None] == slot_range[None, :]).astype(jnp.bfloat16)
    picked = jnp.dot(combine_table, back_flat, preferred_element_type=jnp.float32)
    moe_sum = jnp.sum(
        route_gates[:, :, None] * picked.reshape(seq_count, top_count, model_width), axis=1
    )
    layer_out = (middle.astype(jnp.float32) + rms_scale(moe_sum, out_gain)).astype(jnp.bfloat16)
    return (layer_out, new_state.reshape(seq_count, head_count, HEAD_DIM * HEAD_DIM))


def power_of_two(value):
    return value > 0 and value & (value - 1) == 0


def row_scale(values):
    return values * lax.rsqrt(jnp.mean(values * values, axis=-1, keepdims=True) + norm_eps)


def layer_kernel(
    n,
    m,
    layer_in,
    mix_gain,
    decay_base,
    rate_base,
    key_scale,
    group_gain,
    post_gain,
    ffn_gain,
    out_gain,
    routes,
    route_gates,
    state_hbm,
    rec_hbm,
    key_hbm,
    val_hbm,
    ddown_hbm,
    dup_hbm,
    rdown_hbm,
    rup_hbm,
    out_hbm,
    egate_hbm,
    eup_hbm,
    edown_hbm,
    layer_out,
    new_state,
    state_v,
    proj_v,
    ddown_v,
    dup_v,
    rdown_v,
    rup_v,
    out_v,
    egate_v,
    eup_v,
    edown_v,
    spread_v,
    gather_t,
    products,
    fresh_v,
    s1,
    r1,
    s2,
    r2,
    a3,
    s4,
    p5,
    f6,
    a6,
    s7,
    r7,
    s8,
    r8,
    a9,
    local_sem,
    ep_send,
    ep_recv,
    tp_send,
    tp_recv,
    fw_send,
    fw_recv,
):
    e = lax.axis_index("ep")
    t = lax.axis_index("tp")
    seqs, width = layer_in.shape
    heads = state_hbm.shape[1]
    flat = state_hbm.shape[2]
    cols = rec_hbm.shape[1]
    rows = rec_hbm.shape[0]
    pairs = seqs * heads
    tokens = n * seqs
    f32 = jnp.float32
    bf16 = jnp.bfloat16

    def across(left, right):
        return lax.dot_general(left, right, (((1,), (1,)), ((), ())), preferred_element_type=f32)

    loads = [
        pltpu.make_async_copy(source, target, local_sem.at[i])
        for i, (source, target) in enumerate(
            (
                (ddown_hbm, ddown_v),
                (rdown_hbm, rdown_v),
                (dup_hbm, dup_v),
                (rup_hbm, rup_v),
                (rec_hbm, proj_v.at[0]),
                (key_hbm, proj_v.at[1]),
                (val_hbm, proj_v.at[2]),
                (state_hbm, state_v),
                (out_hbm, out_v),
                (egate_hbm.at[0], egate_v),
                (eup_hbm.at[0], eup_v),
                (edown_hbm.at[0], edown_v),
            )
        )
    ]
    barrier = pltpu.get_barrier_semaphore()
    for d in range(1, n):
        pl.semaphore_signal(barrier, inc=1, device_id=(lax.rem(e + d, n), t), device_id_type=MESH)
    for d in range(1, m):
        pl.semaphore_signal(barrier, inc=1, device_id=(e, lax.rem(t + d, m)), device_id_type=MESH)
    for load in loads:
        load.start()

    def ep_copy(phase, d, source, target):
        return pltpu.make_async_remote_copy(
            src_ref=source,
            dst_ref=target,
            send_sem=ep_send.at[phase, d],
            recv_sem=ep_recv.at[phase, d],
            device_id=(lax.rem(e + d, n), t),
            device_id_type=MESH,
        )

    def tp_copy(phase, d, source, target):
        return pltpu.make_async_remote_copy(
            src_ref=source,
            dst_ref=target,
            send_sem=tp_send.at[phase, d],
            recv_sem=tp_recv.at[phase, d],
            device_id=(e, lax.rem(t + d, m)),
            device_id_type=MESH,
        )

    sent = []

    def start(copies):
        for copy in copies:
            copy.start()
        sent.extend(copies)
        return copies

    token_in = layer_in[...].astype(f32)
    normed = (row_scale(token_in) * mix_gain[...]).astype(bf16)
    for j in range(n):
        s1[j] = normed[:, j * rows : (j + 1) * rows]
    r1[e] = s1[e]
    pl.semaphore_wait(barrier, n - 1 + m - 1)
    first = start([ep_copy(0, d, s1.at[lax.rem(e + d, n)], r1.at[e]) for d in range(1, n)])

    for load in loads[:4]:
        load.wait()
    decay_hidden = jnp.tanh(across(normed, ddown_v[...])).astype(bf16)
    rate_hidden = across(normed, rdown_v[...]).astype(bf16)
    decay_pre = decay_base[...] + jnp.dot(decay_hidden, dup_v[...], preferred_element_type=f32)
    rate_pre = rate_base[...] + jnp.dot(rate_hidden, rup_v[...], preferred_element_type=f32)
    scale_wide = jnp.broadcast_to(key_scale[...], (seqs, cols))

    def head_major(values):
        return jnp.concatenate(
            [values[:, h * HEAD_DIM : (h + 1) * HEAD_DIM] for h in range(heads)], axis=0
        )

    head_bits = int(math.log2(heads))
    seq_bits = int(math.log2(seqs))
    dim_bits = int(math.log2(HEAD_DIM))
    i0 = lax.broadcasted_iota(jnp.int32, (pairs, pairs), 0)
    i1 = lax.broadcasted_iota(jnp.int32, (pairs, pairs), 1)
    to_pairs = (i1 == ((i0 & (heads - 1)) << seq_bits) + (i0 >> head_bits)).astype(f32)
    from_pairs = (i0 == ((i1 & (heads - 1)) << seq_bits) + (i1 >> head_bits)).astype(bf16)

    side = jnp.concatenate(
        [head_major(decay_pre), head_major(rate_pre), head_major(scale_wide)], axis=1
    )
    side = jnp.dot(to_pairs, side, preferred_element_type=f32, precision=lax.Precision.HIGHEST)
    decay = jnp.exp(jax.nn.sigmoid(side[:, :HEAD_DIM]) * -math.exp(-0.5))
    rate = jax.nn.sigmoid(side[:, HEAD_DIM : 2 * HEAD_DIM])
    scale = side[:, 2 * HEAD_DIM :]
    c0 = lax.broadcasted_iota(jnp.int32, (2 * HEAD_DIM, flat), 0) & (HEAD_DIM - 1)
    c1 = lax.broadcasted_iota(jnp.int32, (2 * HEAD_DIM, flat), 1) >> dim_bits
    spread_v[...] = (c0 == c1).astype(f32).astype(bf16)
    g0 = lax.broadcasted_iota(jnp.int32, (flat, HEAD_DIM), 0) >> dim_bits
    g1 = lax.broadcasted_iota(jnp.int32, (flat, HEAD_DIM), 1)
    gather_t[...] = (g0 == g1).astype(f32).astype(bf16)

    for load in loads[4:7]:
        load.wait()
    for copy in first:
        copy.wait_recv()
    spread_rows = r1[...].reshape(tokens, rows)
    for w in range(3):
        part = jnp.dot(spread_rows, proj_v[w], preferred_element_type=f32).astype(bf16)
        s2[:, :, w * cols : (w + 1) * cols] = part.reshape(n, seqs, cols)
    r2[e] = s2[e]
    second = start([ep_copy(1, d, s2.at[lax.rem(e + d, n)], r2.at[e]) for d in range(1, n)])
    loads[7].wait()
    for copy in second:
        copy.wait_recv()
    total = r2[0].astype(f32)
    for j in range(1, n):
        total = total + r2[j].astype(f32)
    total = total.astype(bf16).astype(f32)
    heads_in = jnp.concatenate(
        [head_major(total[:, w * cols : (w + 1) * cols]) for w in range(3)], axis=1
    ).astype(bf16)
    heads_in = jnp.dot(to_pairs.astype(bf16), heads_in, preferred_element_type=f32)
    rec = heads_in[:, :HEAD_DIM]
    key = heads_in[:, HEAD_DIM : 2 * HEAD_DIM]
    val = heads_in[:, 2 * HEAD_DIM :]
    scaled = key * scale
    unit = scaled * lax.rsqrt(jnp.sum(scaled * scaled, axis=-1, keepdims=True) + norm_eps)
    unit_rate = unit * rate
    key_rate = key * rate
    decay_rec = decay * rec
    along_gain = jnp.sum(unit_rate * rec, axis=-1, keepdims=True)
    val_gain = jnp.sum(key_rate * rec, axis=-1, keepdims=True)

    lanes = 2 * HEAD_DIM
    two = lambda values: jnp.concatenate([values, values], axis=1)
    unit2, decay_rec2 = two(unit), two(decay_rec)

    def products_step(j, carry):
        for piece in range(4):
            at = pl.ds(pl.multiple_of((4 * j + piece) * lanes, lanes), lanes)
            block = state_v[:, :, at].reshape(pairs, lanes)
            for i, factor in enumerate((unit2, decay_rec2)):
                value = block * factor
                high = value.astype(bf16)
                products[2 * i * pairs : (2 * i + 1) * pairs, at] = high
                products[(2 * i + 1) * pairs : (2 * i + 2) * pairs, at] = (
                    value - high.astype(f32)
                ).astype(bf16)
        return carry

    lax.fori_loop(0, flat // lanes // 4, products_step, 0)
    reduced = jnp.dot(products[...], gather_t[...], preferred_element_type=f32)
    along = reduced[:pairs] + reduced[pairs : 2 * pairs]
    readout = (
        reduced[2 * pairs : 3 * pairs] + reduced[3 * pairs :] - along * along_gain + val * val_gain
    )
    centred = readout - jnp.mean(readout, axis=-1, keepdims=True)
    normed_out = centred * lax.rsqrt(jnp.mean(centred * centred, axis=-1, keepdims=True) + group_eps)
    out_high = normed_out.astype(bf16)
    out_low = (normed_out - out_high.astype(f32)).astype(bf16)
    back = jnp.dot(
        from_pairs, jnp.concatenate([out_high, out_low], axis=1), preferred_element_type=f32
    )
    back = back[:, :HEAD_DIM] + back[:, HEAD_DIM:]
    back = jnp.concatenate([back[h * seqs : (h + 1) * seqs] for h in range(heads)], axis=1)
    a3[e] = (back * group_gain[...]).astype(bf16)
    third = start([ep_copy(2, d, a3.at[e], a3.at[e]) for d in range(1, n)])

    along_high = along.astype(bf16)
    along_low = (along - along_high.astype(f32)).astype(bf16)
    along_pair = jnp.concatenate([along_high, along_low], axis=1)
    val_low = val.astype(bf16)
    decay2, unit_rate2, key_rate2 = two(decay), two(unit_rate), two(key_rate)

    def fresh_step(j, carry):
        whole = pl.ds(pl.multiple_of(4 * j * lanes, 4 * lanes), 4 * lanes)
        table = spread_v[:, whole]
        along_wide = jnp.dot(along_pair, table, preferred_element_type=f32)
        val_wide = jnp.dot(val_low, table[:HEAD_DIM], preferred_element_type=f32)
        for piece in range(4):
            at = pl.ds(pl.multiple_of((4 * j + piece) * lanes, lanes), lanes)
            block = state_v[:, :, at].reshape(pairs, lanes)
            cut = slice(piece * lanes, (piece + 1) * lanes)
            fresh = (
                block * decay2 - along_wide[:, cut] * unit_rate2 + val_wide[:, cut] * key_rate2
            )
            fresh_v[:, :, at] = fresh.reshape(seqs, heads, lanes)
        return carry

    lax.fori_loop(0, flat // lanes // 4, fresh_step, 0)
    store = pltpu.make_async_copy(fresh_v, new_state, local_sem.at[len(loads)])
    store.start()

    loads[8].wait()
    for copy in third:
        copy.wait_recv()
    part = jnp.dot(a3[...].reshape(tokens, cols), out_v[...], preferred_element_type=f32)
    s4[...] = part.astype(bf16).reshape(n, seqs, rows)
    p5[t, e] = s4[e]
    fourth = start([ep_copy(3, d, s4.at[lax.rem(e + d, n)], p5.at[t, e]) for d in range(1, n)])
    for copy in fourth:
        copy.wait_recv()
    fifth = start([tp_copy(0, d, p5.at[t], p5.at[t]) for d in range(1, m)])
    for copy in fifth:
        copy.wait_recv()
    mixed = p5[0].astype(f32)
    for q in range(1, m):
        mixed = mixed + p5[q].astype(f32)
    mixed = jnp.concatenate([mixed[j] for j in range(n)], axis=1)
    middle = (token_in + row_scale(mixed) * post_gain[...]).astype(bf16).astype(f32)
    ffn_in = (row_scale(middle) * ffn_gain[...]).astype(bf16)

    for q in range(m):
        f6[q] = ffn_in[:, q * cols : (q + 1) * cols]
        a6[q, e] = ffn_in[:, q * cols : (q + 1) * cols]
    sixth = start([ep_copy(4, d, f6.at[t], a6.at[t, e]) for d in range(1, n)])
    near = t + 1 - 2 * lax.rem(t, 2)
    far = lax.rem(t + 2, m)
    cross = lax.rem(near + 2, m)

    def pass_on(kind, d, quarter, target):
        source = lax.rem(e + n - d, n)
        copy = pltpu.make_async_remote_copy(
            src_ref=a6.at[quarter, source],
            dst_ref=a6.at[quarter, source],
            send_sem=fw_send.at[d, kind],
            recv_sem=fw_recv.at[d, kind],
            device_id=(e, target),
            device_id_type=MESH,
        )
        return start([copy])[0]

    to_far, to_near, relayed = [], [], []
    for d in range(1, n):
        sixth[d - 1].wait_recv()
        to_far.append(pass_on(0, d, t, far))
        to_near.append(pass_on(1, d, t, near))
    for load in loads[9:]:
        load.wait()

    def expand(q, gate, up):
        taken = a6[q].reshape(tokens, cols)
        at = pl.ds(pl.multiple_of(q * cols, cols), cols)
        gate = gate + jnp.dot(taken, egate_v[at, :], preferred_element_type=f32)
        up = up + jnp.dot(taken, eup_v[at, :], preferred_element_type=f32)
        return gate, up

    gate = jnp.zeros((tokens, egate_hbm.shape[2]), f32)
    gate, up = expand(t, gate, gate)
    for d in range(1, n):
        to_far[d - 1].wait_recv()
        relayed.append(pass_on(2, d, far, near))
    gate, up = expand(far, gate, up)
    for copy in to_near:
        copy.wait_recv()
    gate, up = expand(near, gate, up)
    for copy in relayed:
        copy.wait_recv()
    gate, up = expand(cross, gate, up)
    gate = jnp.minimum(gate, clamp_limit)
    up = jnp.clip(up, -clamp_limit, clamp_limit)
    hidden = ((up + 1.0) * gate * jax.nn.sigmoid(gate_alpha * gate)).astype(bf16)

    def partial_of(q):
        at = pl.ds(pl.multiple_of(q * cols, cols), cols)
        return jnp.dot(hidden, edown_v[:, at], preferred_element_type=f32).astype(bf16)

    def share(kind, source, target, place):
        copy = pltpu.make_async_remote_copy(
            src_ref=source,
            dst_ref=place,
            send_sem=fw_send.at[0, kind],
            recv_sem=fw_recv.at[0, kind],
            device_id=(e, target),
            device_id_type=MESH,
        )
        return start([copy])[0]

    s7[0] = partial_of(cross)
    far_share = share(0, s7.at[0], near, r7.at[0])
    s7[1] = partial_of(near)
    own_share = share(1, s7.at[1], near, r7.at[1])
    far_sum = partial_of(far).astype(f32)
    far_share.wait_recv()
    s7[2] = (far_sum + r7[0].astype(f32)).astype(bf16)
    last_share = share(2, s7.at[2], far, r7.at[2])
    own = partial_of(t).astype(f32)
    own_share.wait_recv()
    own = own + r7[1].astype(f32)
    last_share.wait_recv()
    own = own + r7[2].astype(f32)
    s8[...] = own.astype(bf16).reshape(n, seqs, cols)
    r8[e] = s8[e]
    eighth = start([ep_copy(5, d, s8.at[lax.rem(e + d, n)], r8.at[e]) for d in range(1, n)])
    named = routes[...]
    gates = route_gates[...]
    same = lax.broadcasted_iota(jnp.int32, (seqs, seqs), 0) == lax.broadcasted_iota(
        jnp.int32, (seqs, seqs), 1
    )
    weights = []
    for j in range(n):
        weight = jnp.sum(jnp.where(named == j, gates, 0.0), axis=0, keepdims=True)
        weight = jnp.where(same, jnp.broadcast_to(weight, (seqs, seqs)), 0.0)
        weights.append(jnp.sum(weight, axis=1, keepdims=True))
    for copy in eighth:
        copy.wait_recv()
    moe = jnp.zeros((seqs, cols), f32)
    for j in range(n):
        moe = moe + weights[j] * r8[j].astype(f32)
    a9[t] = moe.astype(bf16)
    ninth = start([tp_copy(1, d, a9.at[t], a9.at[t]) for d in range(1, m)])
    for copy in ninth:
        copy.wait_recv()
    moe = jnp.concatenate([a9[q] for q in range(m)], axis=1).astype(f32)
    layer_out[...] = (middle + row_scale(moe) * out_gain[...]).astype(bf16)
    for copy in sent:
        copy.wait_send()
    store.wait()


def fused_local(n, m, *args):
    (
        layer_in, state_in, mix_gain, rec_weight, key_weight, val_weight, decay_down, decay_up,
        decay_base, rate_down, rate_up, rate_base, key_scale, group_gain, out_weight, post_gain,
        ffn_gain, routes, route_gates, expert_gate, expert_up, expert_down, out_gain,
    ) = args
    seqs, width = layer_in.shape
    heads, flat = state_in.shape[1:]
    rows, cols = rec_weight.shape
    low = decay_down.shape[1]
    hidden = expert_gate.shape[2]
    pairs = seqs * heads
    tokens = n * seqs
    f32, bf16 = jnp.float32, jnp.bfloat16
    line = lambda values: values.reshape(1, -1)
    vmem = pl.BlockSpec(memory_space=pltpu.VMEM)
    hbm = pl.BlockSpec(memory_space=pl.ANY)
    dma = pltpu.SemaphoreType.DMA
    results = pl.pallas_call(
        functools.partial(layer_kernel, n, m),
        out_shape=(
            jax.ShapeDtypeStruct(layer_in.shape, bf16),
            jax.ShapeDtypeStruct(state_in.shape, f32),
        ),
        in_specs=[vmem] * 11 + [hbm] * 12,
        out_specs=(vmem, hbm),
        scratch_shapes=[
            pltpu.VMEM(state_in.shape, f32),
            pltpu.VMEM((3, rows, cols), bf16),
            pltpu.VMEM((low, width), bf16),
            pltpu.VMEM((low, cols), bf16),
            pltpu.VMEM((low, width), bf16),
            pltpu.VMEM((low, cols), bf16),
            pltpu.VMEM(out_weight.shape, bf16),
            pltpu.VMEM((width, hidden), bf16),
            pltpu.VMEM((width, hidden), bf16),
            pltpu.VMEM((hidden, width), bf16),
            pltpu.VMEM((2 * HEAD_DIM, flat), bf16),
            pltpu.VMEM((flat, HEAD_DIM), bf16),
            pltpu.VMEM((4 * pairs, flat), bf16),
            pltpu.VMEM(state_in.shape, f32),
            pltpu.VMEM((n, seqs, rows), bf16),
            pltpu.VMEM((n, seqs, rows), bf16),
            pltpu.VMEM((n, seqs, 3 * cols), bf16),
            pltpu.VMEM((n, seqs, 3 * cols), bf16),
            pltpu.VMEM((n, seqs, cols), bf16),
            pltpu.VMEM((n, seqs, rows), bf16),
            pltpu.VMEM((m, n, seqs, rows), bf16),
            pltpu.VMEM((m, seqs, cols), bf16),
            pltpu.VMEM((m, n, seqs, cols), bf16),
            pltpu.VMEM((3, tokens, cols), bf16),
            pltpu.VMEM((3, tokens, cols), bf16),
            pltpu.VMEM((n, seqs, cols), bf16),
            pltpu.VMEM((n, seqs, cols), bf16),
            pltpu.VMEM((m, seqs, cols), bf16),
            dma((13,)),
            dma((6, n)),
            dma((6, n)),
            dma((3, m)),
            dma((3, m)),
            dma((n, m)),
            dma((n, m)),
        ],
        compiler_params=pltpu.CompilerParams(
            collective_id=0, has_side_effects=True, vmem_limit_bytes=60 * 1024 * 1024
        ),
    )(
        layer_in, line(mix_gain), line(decay_base), line(rate_base), line(key_scale),
        line(group_gain), line(post_gain), line(ffn_gain), line(out_gain), routes.T, route_gates.T,
        state_in, rec_weight, key_weight, val_weight, decay_down.T, decay_up, rate_down.T, rate_up,
        out_weight, expert_gate, expert_up, expert_down,
    )
    return pl.pallas_call(
        hand_over,
        out_shape=(
            jax.ShapeDtypeStruct(layer_in.shape, bf16),
            jax.ShapeDtypeStruct(state_in.shape, f32),
        ),
        in_specs=[hbm, hbm],
        out_specs=(hbm, hbm),
        scratch_shapes=[
            pltpu.VMEM(layer_in.shape, bf16),
            pltpu.VMEM(state_in.shape, f32),
            dma((seqs + 1,)),
            dma((seqs + 1,)),
        ],
        compiler_params=pltpu.CompilerParams(vmem_limit_bytes=60 * 1024 * 1024),
    )(*results)


def hand_over(token_in, state_in, token_out, state_out, token_v, state_v, in_sem, out_sem):
    count = state_in.shape[0]
    reads = [pltpu.make_async_copy(token_in, token_v, in_sem.at[count])]
    writes = [pltpu.make_async_copy(token_v, token_out, out_sem.at[count])]
    step = 2
    for i in range(0, count, step):
        at = pl.ds(i, step)
        reads.append(pltpu.make_async_copy(state_in.at[at], state_v.at[at], in_sem.at[i]))
        writes.append(pltpu.make_async_copy(state_v.at[at], state_out.at[at], out_sem.at[i]))
    for copy in reads:
        copy.start()
    for read, write in zip(reads, writes):
        read.wait()
        write.start()
    for copy in writes:
        copy.wait()


def choose(n, m, *args):
    seqs, width = args[0].shape
    heads = args[1].shape[1]
    cols = args[3].shape[1]
    experts = args[19].shape[0]
    capacity = max(2, 2 * seqs * args[17].shape[1] // (n * experts))
    if (
        capacity >= seqs
        and experts == 1
        and power_of_two(seqs)
        and power_of_two(heads)
        and seqs % 16 == 0
        and heads % 8 == 0
        and cols * m == width
        and m == 4
        and args[1].shape[2] % (8 * HEAD_DIM) == 0
    ):
        return fused_local(n, m, *args)
    return local(*args)


def solution(mesh):
    in_specs = (
        P("ep", None),
        P("ep", "tp", None),
        P(),
        P("ep", "tp"),
        P("ep", "tp"),
        P("ep", "tp"),
        P(),
        P(None, "tp"),
        P("tp"),
        P(),
        P(None, "tp"),
        P("tp"),
        P("tp"),
        P("tp"),
        P("tp", "ep"),
        P(),
        P(),
        P("ep", None),
        P("ep", None),
        P("ep", None, "tp"),
        P("ep", None, "tp"),
        P("ep", "tp", None),
        P(),
    )
    out_specs = (P("ep", None), P("ep", "tp", None))
    return jax.shard_map(
        functools.partial(choose, mesh.shape["ep"], mesh.shape["tp"]), mesh=mesh, in_specs=in_specs, out_specs=out_specs, check_vma=False)
```
